32 devices in a mesh: fs: 16 (over z, y, x), tp: 2 (over core).
Axes of the slice: x: 2, y: 2, z: 4, core: 2. Of those that a mesh axis runs over, the one named last changes fastest.
Arguments:
- tokens: bfloat16 [2048, 2048], P('fs', 'tp'), may hold values from -300 to 300
- norm_gain: float32 [2048], P('fs'), may hold values from 0.1 to 1.9
- gate_weight: float32 [16, 2048, 1024], P(None, 'fs', 'tp'), may hold values from -1.3258252 to 1.3258252
- up_weight: float32 [16, 2048, 1024], P(None, 'fs', 'tp'), may hold values from -1.3258252 to 1.3258252
- down_weight: float32 [16, 1024, 2048], P(None, 'fs', 'tp'), may hold values from -0.1875 to 0.1875
- routes: int32 [2048, 4], P('fs'), may hold values from 0 to 15, all different within a row; in each aligned block of 128 rows (0 to 127, 128 to 255, ...) at most 64 rows name the same one
- route_weights: float32 [2048, 4], P('fs'), may hold values from 0.05 to 1
Outputs:
- mixed: bfloat16 [2048, 2048], P('fs', 'tp')
- gate_ready: bfloat16 [16, 2048, 1024], P('fs', None, 'tp')
- up_ready: bfloat16 [16, 2048, 1024], P('fs', None, 'tp')
- down_ready: bfloat16 [16, 1024, 2048], P('fs', None, 'tp')
The draws below stay inside these ranges and needn't reach their ends.
Inputs may be any that keep to these rules, and one draw needn't show every extreme that they name: `routes`: each row names 4 different experts. In each aligned block of 128 rows no expert is named more than 64 times, a bound that some block reaches.
All inputs are finite; a program needn't handle non-finite values.
Results may differ from the reference program's by a relative error of at most 0.0089.
Values may be sent and summed in bfloat16 or wider, within the bound.
A program may use at most 64 MiB of HBM per device.

```python
import math
import jax
import jax.numpy as jnp
import numpy as np
from jax import lax

D = 2048
FF = 1024
TOP_K = 4
TOK_DEV = 128
EXPERTS = 16
CAP = 64
TOKENS = 2048
N_FS = 16


def expert_matrix(key, salt):
    base = jax.random.fold_in(key, salt)
    noise = jax.random.truncated_normal(jax.random.fold_in(base, 1), -6.0, 6.0, (EXPERTS, D, FF), jnp.float32)
    column = jnp.exp(jax.random.uniform(jax.random.fold_in(base, 2), (EXPERTS, 1, FF), jnp.float32, math.log(0.5), math.log(3.0)))
    return noise * column * D ** (-0.5)


def draw_gate_weight(key, part):
    return expert_matrix(key, 11)


def draw_up_weight(key, part):
    return expert_matrix(key, 12)


def draw_tokens(key, part):
    base = jax.random.fold_in(key, 21)
    rough = jnp.exp(jax.random.uniform(jax.random.fold_in(base, 3), (1, D), jnp.float32, -0.35, 0.35))
    rising = 3.0 ** (jnp.arange(D, dtype=jnp.float32)[None, :] / max(D - 1, 1))
    noise = jax.random.truncated_normal(jax.random.fold_in(base, 1), -6.0, 6.0, (TOKENS, D), jnp.float32)
    scales = jnp.exp(jax.random.uniform(jax.random.fold_in(base, 2), (TOKENS, 1), jnp.float32, 0.0, math.log(10.0)))
    return (noise * scales * rising * rough).astype(jnp.bfloat16)


def block_levels(rng, dims, split, smallest, largest):
    loudness = 1.0
    for axis_at, shards_of in split:
        draws = jax.random.uniform(jax.random.fold_in(jax.random.fold_in(rng, 6), axis_at), (shards_of,), jnp.float32, smallest / len(split), largest / len(split))
        loudness = loudness * jnp.repeat(jnp.exp(draws), dims[axis_at] // shards_of).reshape((-1,) + (1,) * (len(dims) - 1 - axis_at))
    return loudness


def assign_block(key, own, number, rows, count, top, bound, skew):
    sequence = jax.random.permutation(key, count)
    packed, ordinary = load_shares(count, rows * top, bound, skew, True), load_shares(count, rows * top, bound, skew, False)
    places = jnp.arange(count)

    def named(sizes, turn):
        used = int((sizes > 0).sum())
        fixed = max(1, used // 4)
        shifted = fixed + (places - fixed + turn * (used - fixed)) % max(1, count - fixed)
        return jnp.zeros((count,), jnp.int32).at[sequence[jnp.where(places < fixed, places, shifted)]].set(jnp.asarray(sizes, jnp.int32))

    sizes = jnp.where(number % 4 == 0, named(packed, number // 4), named(ordinary, number - number // 4 - 1))
    mixed = jax.random.permutation(jax.random.fold_in(own, 3), count)
    source_of, receiver = mixed[0:count // 2 * 2:2], mixed[1:count // 2 * 2:2]
    slack = jnp.minimum(sizes[source_of] - 1, bound - sizes[receiver]) // 2
    slack = jnp.where((source_of == sequence[0]) | (receiver == sequence[0]) | (sizes[receiver] == 0), 0, jnp.maximum(slack, 0))
    shifted = jax.random.randint(jax.random.fold_in(own, 4), (count // 2,), 0, 1 << 20) % (slack + 1)
    sizes = sizes.at[source_of].add(-shifted).at[receiver].add(shifted)
    members = jnp.searchsorted(jnp.cumsum(sizes), jnp.arange(rows * top), side="right").astype(jnp.int32)
    table = members.reshape(top, rows).T
    table = table[jax.random.permutation(jax.random.fold_in(own, 1), rows)]
    turn = jax.random.randint(jax.random.fold_in(own, 2), (rows, 1), 0, top)
    return jnp.take_along_axis(table, (jnp.arange(top)[None, :] + turn) % top, axis=1)


def load_shares(number_of, total, limit, skew, full):
    weights = [(1 << 20) // math.isqrt(rank ** skew) + 1 for rank in range(1, number_of + 1)]
    largest = limit if full else min(limit, max(-(-total // number_of), total * weights[0] // sum(weights)))
    least = 1 if total - largest >= number_of - 1 else 0
    given, rest = [largest] + [least] * (number_of - 1), total - largest - least * (number_of - 1)
    while rest > 0:
        movable = [i for i in range(1, number_of) if given[i] < largest] or [i for i in range(1, number_of) if given[i] < limit]
        pool, budget = sum([weights[i] for i in movable]), rest
        for i in movable:
            more = min(limit - given[i], max(1, budget * weights[i] // pool), rest)
            given[i] = given[i] + more
            rest = rest - more
    return np.array(given)


def gaussian(key, extent, width, bound, cuts=(), held_as=jnp.bfloat16):
    factor_of = block_levels(key, extent, cuts, -0.22, 0.18) if cuts else 1.0
    entries = jax.random.normal(key, extent, jnp.float32) * width * factor_of
    return jnp.minimum(jnp.maximum(entries, -bound), bound).astype(held_as)


def setup_inputs(seed: int = 0) -> dict:
    splits = jax.random.split(jax.random.key(seed), 8)
    tokens = draw_tokens(jax.random.fold_in(splits[7], 71), 0)
    norm_gain = jnp.clip(1.0 + 0.18 * jax.random.normal(splits[1], (D,), jnp.float32), 0.1, 1.9)
    gate_weight = draw_gate_weight(jax.random.fold_in(splits[7], 71), 0)
    up_weight = draw_up_weight(jax.random.fold_in(splits[7], 71), 0)
    down_weight = gaussian(splits[4], (EXPERTS, FF, D), FF ** -0.5, 0.1875, ((1, 16), (2, 2)), jnp.float32)
    routes_keys = jax.random.split(jax.random.fold_in(splits[5], 1), TOKENS // TOK_DEV)
    routes_turns = jax.random.permutation(jax.random.fold_in(splits[5], 3), TOKENS // TOK_DEV)
    routes = jax.vmap(lambda own, number: assign_block(jax.random.fold_in(splits[5], 2), own, number, TOK_DEV, EXPERTS, TOP_K, CAP, 2))(routes_keys, routes_turns).reshape((TOKENS, TOP_K))
    route_weights = jnp.clip(jnp.exp(math.log(1.0) - 2.9957323 * jax.random.uniform(splits[6], (TOKENS, TOP_K), jnp.float32) ** block_levels(splits[6], (TOKENS, TOP_K), ((0, 16),), -0.2, 0.2)), 0.05, 1.0)
    return {"tokens": tokens, "norm_gain": norm_gain, "gate_weight": gate_weight, "up_weight": up_weight, "down_weight": down_weight, "routes": routes, "route_weights": route_weights}


epsilon = 1e-05

def activate(gate_pre, up_pre):
    gated = jnp.minimum(gate_pre, 7.0)
    upper = jnp.clip(up_pre, -7.0, 7.0)
    return (upper + 1.0) * gated * jax.nn.sigmoid(1.702 * gated)

def reference(tokens, norm_gain, gate_weight, up_weight, down_weight, routes, route_weights):
    gate_ready = (norm_gain[None, :, None] * gate_weight).astype(jnp.bfloat16)
    up_ready = (norm_gain[None, :, None] * up_weight).astype(jnp.bfloat16)
    down_ready = down_weight.astype(jnp.bfloat16)
    values = tokens.astype(jnp.float32)
    normed = (values * lax.rsqrt(lax.optimization_barrier(jnp.mean(values * values, axis=1, keepdims=True)) + epsilon)).astype(jnp.bfloat16)
    pairs = TOK_DEV * TOP_K
    chosen = routes.reshape(N_FS, pairs)
    onehot = (chosen[:, :, None] == jnp.arange(EXPERTS, dtype=jnp.int32)[None, None, :]).astype(jnp.int32)
    position = lax.optimization_barrier(jnp.sum(jnp.cumsum(onehot, axis=1) * onehot, axis=2)) - 1
    source = jnp.arange(N_FS, dtype=jnp.int32)[:, None]
    row_index = (source * CAP + position).astype(jnp.int32)
    token_index = (source * TOK_DEV + jnp.arange(pairs, dtype=jnp.int32)[None, :] // TOP_K).astype(jnp.int32)
    table = jnp.zeros((EXPERTS, N_FS * CAP), jnp.int32).at[chosen, row_index].set(token_index)

    def expert(operands):
        indices, gate_mat, up_mat, down_mat = operands
        rows = normed[indices]
        gate_pre = jnp.dot(rows, gate_mat, preferred_element_type=jnp.float32)
        up_pre = jnp.dot(rows, up_mat, preferred_element_type=jnp.float32)
        hidden = activate(gate_pre, up_pre).astype(jnp.bfloat16)
        return jnp.dot(hidden, down_mat, preferred_element_type=jnp.float32).astype(jnp.bfloat16)
    outputs = lax.map(expert, (table, gate_ready, up_ready, down_ready))
    picked = outputs[chosen, row_index].astype(jnp.float32).reshape(TOKENS, TOP_K, D)
    mixed = lax.optimization_barrier(jnp.sum(picked * route_weights[:, :, None], axis=1)).astype(jnp.bfloat16)
    return (mixed, gate_ready, up_ready, down_ready)
```

```python
import functools

import jax
import jax.numpy as jnp
from jax import lax
from jax.experimental import pallas as pl
from jax.experimental.pallas import tpu as pltpu
from jax.sharding import PartitionSpec as P

epsilon = 1e-05
MESH = pl.DeviceIdType.MESH
GROUPS = 4


def activate(gate_pre, up_pre):
    gated = jnp.minimum(gate_pre, 7.0)
    upper = jnp.clip(up_pre, -7.0, 7.0)
    return (upper + 1.0) * gated * jax.nn.sigmoid(1.702 * gated)


def kernel(
    n, cores, slots_in, gate_in, up_in, down_in, mix_high, mix_low,
    mixed_out, gate_out, up_out, down_out,
    rows, gate, up, down, hidden, results, back,
    send_sem, recv_sem, own_sem, out_sem, tp_send, tp_recv,
):
    me = lax.axis_index("fs")
    core = lax.axis_index("tp")
    depth = gate_in.shape[1]
    units = down_in.shape[1]
    items = slots_in.shape[1]
    total = n * items
    width = slots_in.shape[2]
    columns = gate_in.shape[2]

    barrier = pltpu.get_barrier_semaphore()

    def greet(step, carry):
        pl.semaphore_signal(barrier, inc=1, device_id={"fs": lax.rem(me + step, n)}, device_id_type=MESH)
        return carry

    lax.fori_loop(1, n, greet, 0)
    for step in range(1, cores):
        pl.semaphore_signal(barrier, inc=1, device_id={"tp": lax.rem(core + step, cores)}, device_id_type=MESH)
    pl.semaphore_wait(barrier, n - 1 + cores - 1)

    mine = rows.at[core]
    phases = ((slots_in, mine, items), (gate_in, gate, depth), (up_in, up, depth), (down_in, down, units))

    def own(phase):
        source, landing, size = phases[phase]
        return pltpu.make_async_copy(source.at[me], landing.at[pl.ds(me * size, size)], own_sem.at[phase])

    def start(phase):
        source, landing, size = phases[phase]

        def send(step, carry):
            peer = lax.rem(me + step, n)
            pltpu.make_async_remote_copy(
                src_ref=source.at[peer],
                dst_ref=landing.at[pl.ds(me * size, size)],
                send_sem=send_sem.at[phase],
                recv_sem=recv_sem.at[phase],
                device_id={"fs": peer},
                device_id_type=MESH,
            ).start()
            return carry

        own(phase).start()
        lax.fori_loop(1, n, send, 0)

    def drain(landing, size, semaphore):
        piece = landing.at[pl.ds(0, (n - 1) * size)]
        pltpu.make_async_copy(piece, piece, semaphore).wait()

    def arrive(phase):
        _, landing, size = phases[phase]
        drain(landing, size, recv_sem.at[phase])
        own(phase).wait()

    def swap(buffer, slot):
        copies = []
        for step in range(1, cores):
            copies.append(
                pltpu.make_async_remote_copy(
                    src_ref=buffer.at[core],
                    dst_ref=buffer.at[core],
                    send_sem=tp_send.at[slot, step - 1],
                    recv_sem=tp_recv.at[slot, step - 1],
                    device_id={"tp": lax.rem(core + step, cores)},
                    device_id_type=MESH,
                )
            )
        for copy in copies:
            copy.start()
        return copies

    for phase in range(4):
        start(phase)

    arrive(0)
    swapped = swap(rows, 0)
    arrive(1)
    gate_copy = pltpu.make_async_copy(gate, gate_out, out_sem.at[0])
    gate_copy.start()
    for copy in swapped:
        copy.wait()
    arrive(2)
    up_copy = pltpu.make_async_copy(up, up_out, out_sem.at[1])
    up_copy.start()

    tile = total // GROUPS

    def first_layer(group, carry):
        at = pl.ds(pl.multiple_of(group * tile, tile), tile)
        gate_pre = jnp.zeros((tile, columns), jnp.float32)
        up_pre = jnp.zeros((tile, columns), jnp.float32)
        for part in range(cores):
            block = rows[part, at, :]
            span = pl.ds(part * width, width)
            gate_pre = gate_pre + jnp.dot(block, gate[span, :], preferred_element_type=jnp.float32)
            up_pre = up_pre + jnp.dot(block, up[span, :], preferred_element_type=jnp.float32)
        hidden[core, at, :] = activate(gate_pre, up_pre).astype(jnp.bfloat16)
        return carry

    lax.fori_loop(0, GROUPS, first_layer, 0)
    swapped = swap(hidden, 1)
    for copy in swapped:
        copy.wait()
    arrive(3)
    down_copy = pltpu.make_async_copy(down, down_out, out_sem.at[2])
    down_copy.start()

    share = n // GROUPS
    home = me // share

    def second_layer(turn, carry):
        group = lax.rem(home + 1 + turn, GROUPS)
        at = pl.ds(pl.multiple_of(group * tile, tile), tile)
        summed = jnp.zeros((tile, width), jnp.float32)
        for part in range(cores):
            summed = summed + jnp.dot(
                hidden[part, at, :], down[pl.ds(part * columns, columns), :], preferred_element_type=jnp.float32
            )
        results[at, :] = summed.astype(jnp.bfloat16)

        def give(step, inner):
            peer = group * share + lax.rem(me + step, share)

            @pl.when(peer != me)
            def _():
                pltpu.make_async_remote_copy(
                    src_ref=results.at[pl.ds(peer * items, items)],
                    dst_ref=back.at[pl.ds(me * items, items)],
                    send_sem=send_sem.at[4],
                    recv_sem=recv_sem.at[4],
                    device_id={"fs": peer},
                    device_id_type=MESH,
                ).start()

            return inner

        lax.fori_loop(0, share, give, 0)
        return carry

    lax.fori_loop(0, GROUPS, second_layer, 0)
    kept = pltpu.make_async_copy(
        results.at[pl.ds(me * items, items)], back.at[pl.ds(me * items, items)], own_sem.at[4]
    )
    kept.start()
    kept.wait()
    gate_copy.wait()
    up_copy.wait()
    down_copy.wait()
    for phase in range(4):
        source, landing, size = phases[phase]
        drain(landing, size, send_sem.at[phase])
    drain(back, items, send_sem.at[4])
    drain(back, items, recv_sem.at[4])
    mixed = jnp.dot(mix_high[...], back[...], preferred_element_type=jnp.float32)
    mixed = mixed + jnp.dot(mix_low[...], back[...], preferred_element_type=jnp.float32)
    mixed_out[...] = mixed.astype(jnp.bfloat16)


def shards(n, cores, tokens, norm_gain, gate_weight, up_weight, down_weight, routes, route_weights):
    experts, depth, columns = gate_weight.shape
    units, width = down_weight.shape[1:]
    tok_rows, top_count = routes.shape
    items = 2 * tok_rows * top_count // experts
    total = experts * items
    gate_send = (norm_gain[None, :, None] * gate_weight).astype(jnp.bfloat16)
    up_send = (norm_gain[None, :, None] * up_weight).astype(jnp.bfloat16)
    down_send = down_weight.astype(jnp.bfloat16)

    values = tokens.astype(jnp.float32)
    squared = lax.psum(jnp.sum(values * values, axis=1), "tp")
    normed = (values * lax.rsqrt(squared / (width * cores) + epsilon)[:, None]).astype(jnp.bfloat16)

    names = jnp.arange(experts, dtype=jnp.int32)
    hits = routes[:, :, None] == names[None, None, :]
    member = jnp.any(hits, axis=1)
    weight = jnp.sum(jnp.where(hits, route_weights[:, :, None], 0.0), axis=1)
    order = jnp.arange(tok_rows, dtype=jnp.int32)
    earlier = (order[:, None] > order[None, :]).astype(jnp.bfloat16)
    place = jnp.dot(earlier, member.astype(jnp.bfloat16), preferred_element_type=jnp.float32).astype(jnp.int32)
    place = jnp.where(member, place, -1)
    slots = jnp.arange(items, dtype=jnp.int32)
    chosen = place.T[:, None, :] == slots[None, :, None]
    picks = chosen.astype(jnp.bfloat16).reshape(total, tok_rows)
    outbound = jnp.dot(picks, normed, preferred_element_type=jnp.float32).astype(jnp.bfloat16)
    rounded = lax.reduce_precision(weight, 8, 7)
    high = rounded.astype(jnp.bfloat16)
    low = (weight - rounded).astype(jnp.bfloat16)
    at_slot = place[:, :, None] == slots[None, None, :]
    zero = jnp.zeros((), jnp.bfloat16)
    mix_high = jnp.where(at_slot, high[:, :, None], zero).reshape(tok_rows, total)
    mix_low = jnp.where(at_slot, low[:, :, None], zero).reshape(tok_rows, total)

    anywhere = pl.BlockSpec(memory_space=pl.ANY)
    near = pl.BlockSpec(memory_space=pltpu.VMEM)
    mixed, gate_ready, up_ready, down_ready = pl.pallas_call(
        functools.partial(kernel, n, cores),
        out_shape=(
            jax.ShapeDtypeStruct((tok_rows, width), jnp.bfloat16),
            jax.ShapeDtypeStruct((n * depth, columns), jnp.bfloat16),
            jax.ShapeDtypeStruct((n * depth, columns), jnp.bfloat16),
            jax.ShapeDtypeStruct((n * units, width), jnp.bfloat16),
        ),
        in_specs=[anywhere] * 4 + [near] * 2,
        out_specs=(near, anywhere, anywhere, anywhere),
        scratch_shapes=[
            pltpu.VMEM((cores, total, width), jnp.bfloat16),
            pltpu.VMEM((n * depth, columns), jnp.bfloat16),
            pltpu.VMEM((n * depth, columns), jnp.bfloat16),
            pltpu.VMEM((n * units, width), jnp.bfloat16),
            pltpu.VMEM((cores, total, columns), jnp.bfloat16),
            pltpu.VMEM((total, width), jnp.bfloat16),
            pltpu.VMEM((total, width), jnp.bfloat16),
            pltpu.SemaphoreType.DMA((5,)),
            pltpu.SemaphoreType.DMA((5,)),
            pltpu.SemaphoreType.DMA((5,)),
            pltpu.SemaphoreType.DMA((3,)),
            pltpu.SemaphoreType.DMA((2, cores - 1)),
            pltpu.SemaphoreType.DMA((2, cores - 1)),
        ],
        compiler_params=pltpu.CompilerParams(
            collective_id=0, has_side_effects=True, vmem_limit_bytes=40 * 1024 * 1024
        ),
    )(outbound.reshape(experts, items, width), gate_send, up_send, down_send, mix_high, mix_low)
    return (mixed, gate_ready[None], up_ready[None], down_ready[None])


def solution(mesh):
    placed = (
        P("fs", "tp"),
        P("fs"),
        P(None, "fs", "tp"),
        P(None, "fs", "tp"),
        P(None, "fs", "tp"),
        P("fs", None),
        P("fs", None),
    )
    return jax.shard_map(
        functools.partial(shards, mesh.shape["fs"], mesh.shape["tp"]),
        mesh=mesh,
        in_specs=placed,
        out_specs=(P("fs", "tp"), P("fs", None, "tp"), P("fs", None, "tp"), P("fs", None, "tp")),
        check_vma=False,
    )
```
